32 devices in a mesh: pp: 4 (over z), fs: 4 (over y, x), tp: 2 (over core).
Axes of the slice: x: 2, y: 2, z: 4, core: 2. Of those that a mesh axis runs over, the one named last changes fastest.
Arguments:
- tokens: bfloat16 [4, 8, 128, 2048], P('pp', ('fs', 'tp')), may hold values from -6 to 6
- layer_norm_scale: float32 [4, 2048], P('pp'), may hold values from 0.1 to 1.9
- input_weight: bfloat16 [4, 2048, 1024], P('pp'), may hold values from -0.125 to 0.125
- filter_weight: float32 [4, 4, 1024], P('pp'), may hold values from -3 to 3
- filter_bias: float32 [4, 1024], P('pp'), may hold values from -2 to 2
- recur_gate_weight: bfloat16 [4, 8, 128, 128], P('pp'), may hold values from -0.5 to 0.5
- recur_gate_bias: float32 [4, 1024], P('pp'), may hold values from -4 to 4
- input_gate_weight: bfloat16 [4, 8, 128, 128], P('pp'), may hold values from -0.5 to 0.5
- input_gate_bias: float32 [4, 1024], P('pp'), may hold values from -4 to 4
- decay_setting: float32 [4, 1024], P('pp'), may hold values from -2 to 8
- spike_log_decay: float32 [4, 128], P('pp'), may hold values from -0.7 to 0, as said below
- output_weight: bfloat16 [4, 1024, 2048], P('pp'), may hold values from -0.375 to 0.375
Outputs:
- result: bfloat16 [4, 8, 128, 2048], P('pp', ('fs', 'tp'))
The draws below stay inside these ranges and needn't reach their ends.
Inputs may be any that keep to these rules, and one draw needn't show every extreme that they name: `spike_log_decay`: zero at most positions; at a few positions of each layer drawn from the seed it lies between log(0.5) and log(0.8).
All inputs are finite; a program needn't handle non-finite values.
Results may differ from the reference program's by a relative error of at most 0.023.
Values may be sent and summed in bfloat16 or wider, within the bound.
A program may use at most 64 MiB of HBM per device.

```python
import math
import jax
import jax.numpy as jnp
from jax import lax

D = 2048
RW = 1024
GB = 8
BW = 128
CONV = 4
LEN = 128
SECTIONS = 4
MICRO = 4
SEQS = 8


def draw_spike_log_decay(key, part):
    marks = jax.random.randint(jax.random.fold_in(key, 11), (SECTIONS, LEN), 0, LEN) < 3
    values = jax.random.uniform(jax.random.fold_in(key, 12), (SECTIONS, LEN), jnp.float32, math.log(0.5), math.log(0.8))
    return jnp.where(marks, values, 0.0).astype(jnp.float32)


def draw_decay_setting(key, part):
    fast_share = 0.6
    fast_low = -1.5
    fast_high = 0.5
    picks = jax.random.uniform(jax.random.fold_in(key, 21), (SECTIONS, RW), jnp.float32)
    quick = jax.random.uniform(jax.random.fold_in(key, 22), (SECTIONS, RW), jnp.float32, fast_low, fast_high)
    slow = jax.random.uniform(jax.random.fold_in(key, 23), (SECTIONS, RW), jnp.float32, 6.0, 8.0)
    return jnp.where(picks < fast_share, quick, slow).astype(jnp.float32)


def steps_of(stream_key, dims, split, least, largest):
    loudness = 1.0
    for position, parts in split:
        draws = jax.random.uniform(jax.random.fold_in(jax.random.fold_in(stream_key, 6), position), (parts,), jnp.float32, least / len(split), largest / len(split))
        loudness = loudness * jnp.repeat(jnp.exp(draws), dims[position] // parts).reshape((-1,) + (1,) * (len(dims) - 1 - position))
    return loudness


def bell_draw(stream_key, dims, spread, limit, shards=(), kind=jnp.bfloat16):
    drawn = spread * jax.random.normal(stream_key, dims, jnp.float32)
    if shards:
        drawn = drawn * steps_of(stream_key, dims, shards, -0.22, 0.18)
    return jnp.clip(drawn, -limit, limit).astype(kind)


def setup_inputs(seed: int = 0) -> dict:
    arg_keys = jax.random.split(jax.random.key(seed), 13)
    tokens = bell_draw(arg_keys[0], (MICRO, SEQS, LEN, D), 1.0, 6.0, ((0, 4), (1, 8)))
    layer_norm_scale = jnp.clip(1.0 + 0.18 * jax.random.normal(arg_keys[1], (SECTIONS, D), jnp.float32), 0.1, 1.9)
    input_weight = bell_draw(arg_keys[2], (SECTIONS, D, RW), D ** -0.5, 0.125, ((0, 4),))
    filter_weight = bell_draw(arg_keys[3], (SECTIONS, CONV, RW), CONV ** -0.5, 3.0, ((0, 4),), jnp.float32)
    filter_bias = bell_draw(arg_keys[4], (SECTIONS, RW), 0.3, 2.0, ((0, 4),), jnp.float32)
    recur_gate_weight = bell_draw(arg_keys[5], (SECTIONS, GB, BW, BW), BW ** -0.5, 0.5, ((0, 4),))
    recur_gate_bias = bell_draw(arg_keys[6], (SECTIONS, RW), 1.0, 4.0, ((0, 4),), jnp.float32)
    input_gate_weight = bell_draw(arg_keys[7], (SECTIONS, GB, BW, BW), BW ** -0.5, 0.5, ((0, 4),))
    input_gate_bias = bell_draw(arg_keys[8], (SECTIONS, RW), 1.0, 4.0, ((0, 4),), jnp.float32)
    decay_setting = draw_decay_setting(jax.random.fold_in(arg_keys[12], 71), 0)
    spike_log_decay = draw_spike_log_decay(jax.random.fold_in(arg_keys[12], 71), 0)
    output_weight = bell_draw(arg_keys[11], (SECTIONS, RW, D), (RW // 4) ** -0.5, 0.375, ((0, 4),))
    return {"tokens": tokens, "layer_norm_scale": layer_norm_scale, "input_weight": input_weight, "filter_weight": filter_weight, "filter_bias": filter_bias, "recur_gate_weight": recur_gate_weight, "recur_gate_bias": recur_gate_bias, "input_gate_weight": input_gate_weight, "input_gate_bias": input_gate_bias, "decay_setting": decay_setting, "spike_log_decay": spike_log_decay, "output_weight": output_weight}


def combine_pair(left, right):
    return (left[0] * right[0], right[0] * left[1] + right[1])

def one_layer(hidden, weight_bundle):
    norm_factor, input_projected, filter_kernel_taps, filter_offset, retention_weight, retention_bias, injection_weight, injection_bias, unscaled_decay, decay_spike, output_projected = weight_bundle
    batch = hidden.shape[0]
    width = input_projected.shape[1]
    taps = filter_kernel_taps.shape[0]
    blocks = retention_weight.shape[0]
    hidden32 = hidden.astype(jnp.float32)
    squares = lax.optimization_barrier(jnp.mean(hidden32 * hidden32, axis=-1, keepdims=True))
    normed = (hidden32 * lax.rsqrt(squares + 1e-06) * norm_factor).astype(jnp.bfloat16)
    mixed_in = jnp.dot(normed.reshape(-1, normed.shape[-1]), input_projected, preferred_element_type=jnp.float32)
    mixed_in = mixed_in.astype(jnp.bfloat16).reshape(batch, -1, width)
    length = mixed_in.shape[1]
    padded = jnp.pad(mixed_in.astype(jnp.float32), ((0, 0), (taps - 1, 0), (0, 0)))
    conv_out = filter_offset + sum((padded[:, k:k + length] * filter_kernel_taps[k] for k in range(taps)))
    conv_out = conv_out.astype(jnp.bfloat16)
    grouped = conv_out.astype(jnp.float32).reshape(batch * length, blocks, -1)
    retention_gate = jax.nn.sigmoid(jnp.einsum('ngi,gij->ngj', grouped, retention_weight.astype(jnp.float32)).reshape(batch, length, width) + retention_bias)
    inject = jax.nn.sigmoid(jnp.einsum('ngi,gij->ngj', grouped, injection_weight.astype(jnp.float32)).reshape(batch, length, width) + injection_bias)
    decay_logarithm = -8.0 * retention_gate * jax.nn.softplus(-unscaled_decay) + decay_spike[None, :, None]
    decay = jnp.exp(decay_logarithm)
    update = jnp.sqrt(-jnp.expm1(2.0 * decay_logarithm)) * inject * conv_out.astype(jnp.float32)
    states = lax.associative_scan(combine_pair, (decay, update), axis=1)[1].astype(jnp.bfloat16)
    projected = jnp.dot(states.reshape(-1, width), output_projected, preferred_element_type=jnp.float32)
    return (hidden32 + projected.reshape(hidden.shape)).astype(jnp.bfloat16)

def reference(tokens, layer_norm_scale, input_weight, filter_weight, filter_bias, recur_gate_weight, recur_gate_bias, input_gate_weight, input_gate_bias, decay_setting, spike_log_decay, output_weight):
    hidden = tokens.reshape(-1, tokens.shape[2], tokens.shape[3])

    def advance(carry, weight_bundle):
        return (one_layer(carry, weight_bundle), None)
    layer_stacked_params = (layer_norm_scale, input_weight, filter_weight, filter_bias, recur_gate_weight, recur_gate_bias, input_gate_weight, input_gate_bias, decay_setting, spike_log_decay, output_weight)
    hidden, unused = lax.scan(advance, hidden, layer_stacked_params)
    return hidden.reshape(tokens.shape)
```

```python
import functools

import jax
import jax.numpy as jnp
from jax import lax
from jax.experimental import pallas as pl
from jax.experimental.pallas import tpu as pltpu
from jax.sharding import PartitionSpec as P

MESH = pl.DeviceIdType.MESH
CHUNKS = 4
GROUP = 8
LANES = 128


def one_minus_exp(y):
    series = -y * (1.0 + y * (0.5 + y * (1.0 / 6.0 + y * (1.0 / 24.0 + y * (1.0 / 120.0)))))
    return jnp.where(y > -0.25, series, 1.0 - jnp.exp(y))


def kernel(
    stages,
    chunks,
    tokens,
    scale,
    w_in_hbm,
    taps,
    tap_bias,
    gr_hbm,
    bias_r,
    gi_hbm,
    bias_i,
    decay_setting,
    spike,
    w_out_hbm,
    out,
    x_in,
    y_out,
    landed,
    w_in,
    w_out,
    gates,
    tails,
    carries,
    rates,
    spikes,
    states,
    in_sem,
    send_sem,
    tok_sem,
    res_sem,
    w_sem,
    out_sem,
):
    me = lax.axis_index("pp")
    last = stages - 1
    length, width = tokens.shape
    rows = length // chunks
    channels = w_in.shape[1]
    blocks = gates.shape[0]
    ntaps = taps.shape[0]

    def chunk_rows(c):
        return pl.ds(pl.multiple_of(c * rows, rows), rows)

    def token_copy(c):
        return pltpu.make_async_remote_copy(
            src_ref=tokens.at[chunk_rows(c)],
            dst_ref=x_in.at[me, c],
            send_sem=tok_sem.at[c],
            recv_sem=in_sem.at[me, c],
            device_id={"pp": 0},
            device_id_type=MESH,
        )

    def forward_copy(m, c):
        return pltpu.make_async_remote_copy(
            src_ref=y_out.at[m, c],
            dst_ref=x_in.at[m, c],
            send_sem=send_sem.at[m, c],
            recv_sem=in_sem.at[m, c],
            device_id={"pp": me + 1},
            device_id_type=MESH,
        )

    def home_copy(m, c):
        return pltpu.make_async_remote_copy(
            src_ref=y_out.at[m, c],
            dst_ref=landed.at[c],
            send_sem=send_sem.at[m, c],
            recv_sem=res_sem.at[c],
            device_id={"pp": m},
            device_id_type=MESH,
        )

    weight_copies = [
        pltpu.make_async_copy(w_in_hbm, w_in, w_sem.at[0]),
        pltpu.make_async_copy(gr_hbm, gates.at[:, :, pl.ds(0, LANES)], w_sem.at[1]),
        pltpu.make_async_copy(gi_hbm, gates.at[:, :, pl.ds(LANES, LANES)], w_sem.at[2]),
        pltpu.make_async_copy(w_out_hbm, w_out, w_sem.at[3]),
    ]

    barrier = pltpu.get_barrier_semaphore()
    for step in range(1, stages):
        pl.semaphore_signal(
            barrier, inc=1, device_id={"pp": lax.rem(me + step, stages)}, device_id_type=MESH
        )

    @pl.when(me == 0)
    def _():
        for c in range(chunks):
            pltpu.make_async_copy(tokens.at[chunk_rows(c)], x_in.at[0, c], in_sem.at[0, c]).start()

    for copy in weight_copies:
        copy.start()
    rates[...] = -8.0 * (
        jnp.maximum(-decay_setting[...], 0.0)
        + jnp.log1p(jnp.exp(-jnp.abs(decay_setting[...])))
    )
    spikes[...] = jnp.broadcast_to(spike[...], (LANES, length)).T
    tails[...] = jnp.zeros_like(tails)
    carries[...] = jnp.zeros_like(carries)
    pl.semaphore_wait(barrier, stages - 1)

    @pl.when(me > 0)
    def _():
        for c in range(chunks):
            token_copy(c).start()

    for copy in weight_copies:
        copy.wait()

    def layer(m, c):
        hidden = x_in[m, c].astype(jnp.float32)
        squares = jnp.mean(hidden * hidden, axis=-1, keepdims=True)
        normed = (hidden * lax.rsqrt(squares + 1e-6) * scale[...]).astype(jnp.bfloat16)
        row_in_group = lax.broadcasted_iota(jnp.int32, (rows // GROUP, GROUP, LANES), 1)
        spiked = spikes[chunk_rows(c), :]
        pair = 2 * LANES
        for two in range(channels // pair):
            wide = slice(two * pair, (two + 1) * pair)
            mixed = jnp.dot(normed, w_in[:, wide], preferred_element_type=jnp.float32)
            mixed = mixed.astype(jnp.bfloat16).astype(jnp.float32)
            padded = jnp.concatenate([tails[m, :, wide], mixed], axis=0)
            tails[m, :, wide] = mixed[rows - GROUP :]
            conv = tap_bias[:, wide]
            for k in range(ntaps):
                start = GROUP - (ntaps - 1) + k
                conv = conv + padded[start : start + rows] * taps[k : k + 1, wide]
            conv = conv.astype(jnp.bfloat16)
            for half in range(2):
                g = 2 * two + half
                lanes = slice(g * LANES, (g + 1) * LANES)
                mine = conv[:, half * LANES : (half + 1) * LANES]
                z = jnp.dot(mine, gates[g], preferred_element_type=jnp.float32)
                recall = jax.nn.sigmoid(z[:, :LANES] + bias_r[:, lanes])
                inject = jax.nn.sigmoid(z[:, LANES:] + bias_i[:, lanes])
                log_decay = recall * rates[:, lanes] + spiked
                a = jnp.exp(log_decay)
                u = jnp.sqrt(one_minus_exp(2.0 * log_decay)) * inject * mine.astype(jnp.float32)
                a = a.reshape(rows // GROUP, GROUP, LANES)
                u = u.reshape(rows // GROUP, GROUP, LANES)
                for by in (1, 2, 4):
                    inside = row_in_group >= by
                    u = u + a * jnp.where(inside, pltpu.roll(u, by, 1), 0.0)
                    a = a * jnp.where(inside, pltpu.roll(a, by, 1), 1.0)
                carry = carries[m, :, lanes]
                parts = []
                for i in range(rows // GROUP):
                    h = a[i] * carry + u[i]
                    parts.append(h)
                    carry = jnp.broadcast_to(h[GROUP - 1 :], (GROUP, LANES))
                carries[m, :, lanes] = carry
                states[:, lanes] = jnp.concatenate(parts, axis=0).astype(jnp.bfloat16)
        projected = jnp.dot(states[...], w_out[...], preferred_element_type=jnp.float32)
        y_out[m, c] = (x_in[m, c].astype(jnp.float32) + projected).astype(jnp.bfloat16)

    def advance(i, _):
        j = jnp.maximum(i - chunks, 0)
        others = max(stages - 1, 1)
        first = i < chunks
        m = jnp.where(first, 0, 1 + j % others)
        c = jnp.where(first, i, j // others)
        pltpu.make_async_copy(x_in.at[m, c], x_in.at[m, c], in_sem.at[m, c]).wait()
        layer(m, c)

        @pl.when(me < last)
        def _():
            forward_copy(m, c).start()

        @pl.when((me == last) & (m < last))
        def _():
            home_copy(m, c).start()

        return 0

    lax.fori_loop(0, stages * chunks, advance, 0)

    def final_copy(source, c):
        return pltpu.make_async_copy(source, out.at[chunk_rows(c)], out_sem.at[c])

    @pl.when(me == last)
    def _():
        for c in range(chunks):
            final_copy(y_out.at[last, c], c).start()

    @pl.when(me < last)
    def _():
        for c in range(chunks):
            pltpu.make_async_copy(landed.at[c], landed.at[c], res_sem.at[c]).wait()
            final_copy(landed.at[c], c).start()

    @pl.when(me > 0)
    def _():
        for c in range(chunks):
            token_copy(c).wait_send()

    def drain(i, _):
        m = i // chunks
        c = i % chunks

        @pl.when(me < last)
        def _():
            forward_copy(m, c).wait_send()

        @pl.when((me == last) & (m < last))
        def _():
            home_copy(m, c).wait_send()

        return 0

    lax.fori_loop(0, stages * chunks, drain, 0)
    for c in range(chunks):
        final_copy(landed.at[c], c).wait()


def solution(mesh):
    stages = mesh.shape["pp"]

    def local(
        tokens, norm, w_in, taps, tap_bias, gr, br, gi, bi, decay_setting, spike, w_out
    ):
        length, width = tokens.shape[2:]
        channels = w_in.shape[2]
        blocks, wide = gr.shape[1:3]
        rows = length // CHUNKS
        vmem = pl.BlockSpec(memory_space=pltpu.VMEM)
        anywhere = pl.BlockSpec(memory_space=pl.ANY)
        result = pl.pallas_call(
            functools.partial(kernel, stages, CHUNKS),
            out_shape=jax.ShapeDtypeStruct((length, width), jnp.bfloat16),
            in_specs=[
                anywhere, vmem, anywhere, vmem, vmem, anywhere, vmem, anywhere, vmem, vmem, vmem,
                anywhere,
            ],
            out_specs=anywhere,
            scratch_shapes=[
                pltpu.VMEM((stages, CHUNKS, rows, width), jnp.bfloat16),
                pltpu.VMEM((stages, CHUNKS, rows, width), jnp.bfloat16),
                pltpu.VMEM((CHUNKS, rows, width), jnp.bfloat16),
                pltpu.VMEM((width, channels), jnp.bfloat16),
                pltpu.VMEM((channels, width), jnp.bfloat16),
                pltpu.VMEM((blocks, wide, 2 * wide), jnp.bfloat16),
                pltpu.VMEM((stages, GROUP, channels), jnp.float32),
                pltpu.VMEM((stages, GROUP, channels), jnp.float32),
                pltpu.VMEM((1, channels), jnp.float32),
                pltpu.VMEM((length, LANES), jnp.float32),
                pltpu.VMEM((rows, channels), jnp.bfloat16),
                pltpu.SemaphoreType.DMA((stages, CHUNKS)),
                pltpu.SemaphoreType.DMA((stages, CHUNKS)),
                pltpu.SemaphoreType.DMA((CHUNKS,)),
                pltpu.SemaphoreType.DMA((CHUNKS,)),
                pltpu.SemaphoreType.DMA((4,)),
                pltpu.SemaphoreType.DMA((CHUNKS,)),
            ],
            compiler_params=pltpu.CompilerParams(
                collective_id=0, has_side_effects=True, vmem_limit_bytes=60 * 1024 * 1024
            ),
        )(
            tokens[0, 0], norm, w_in[0], taps[0], tap_bias, gr[0], br, gi[0], bi, decay_setting,
            spike, w_out[0],
        )
        return result[None, None]

    placed = (
        P("pp", ("fs", "tp"), None, None),
        P("pp", None),
        P("pp", None, None),
        P("pp", None, None),
        P("pp", None),
        P("pp", None, None, None),
        P("pp", None),
        P("pp", None, None, None),
        P("pp", None),
        P("pp", None),
        P("pp", None),
        P("pp", None, None),
    )
    return jax.shard_map(
        local,
        mesh=mesh,
        in_specs=placed,
        out_specs=P("pp", ("fs", "tp"), None, None),
        check_vma=False,
    )
```

```python
import functools

import jax
import jax.numpy as jnp
from jax import lax
from jax.experimental import pallas as pl
from jax.experimental.pallas import tpu as pltpu
from jax.sharding import PartitionSpec as P

MESH = pl.DeviceIdType.MESH
CHUNKS = 4
GO_CHUNK = CHUNKS - 1
DEFER = CHUNKS
GROUP = 8
LANES = 128


def one_minus_exp(y):
    series = -y * (1.0 + y * (0.5 + y * (1.0 / 6.0 + y * (1.0 / 24.0 + y * (1.0 / 120.0)))))
    return jnp.where(y > -0.25, series, 1.0 - jnp.exp(y))


def kernel(
    stages,
    chunks,
    tokens,
    scale,
    w_in_hbm,
    taps,
    tap_bias,
    gr_hbm,
    bias_r,
    gi_hbm,
    bias_i,
    decay_setting,
    spike,
    w_out_hbm,
    out,
    x_in,
    y_out,
    landed,
    w_in,
    w_out,
    gates,
    tails,
    carries,
    rates,
    spikes,
    states,
    in_sem,
    send_sem,
    tok_sem,
    res_sem,
    w_sem,
    out_sem,
    go_sem,
):
    me = lax.axis_index("pp")
    last = stages - 1
    length, width = tokens.shape
    rows = length // chunks
    channels = w_in.shape[1]
    blocks = gates.shape[0]
    ntaps = taps.shape[0]

    def chunk_rows(c):
        return pl.ds(pl.multiple_of(c * rows, rows), rows)

    def token_copy(c):
        return pltpu.make_async_remote_copy(
            src_ref=tokens.at[chunk_rows(c)],
            dst_ref=x_in.at[me, c],
            send_sem=tok_sem.at[c],
            recv_sem=in_sem.at[me, c],
            device_id={"pp": 0},
            device_id_type=MESH,
        )

    def forward_copy(m, c):
        return pltpu.make_async_remote_copy(
            src_ref=y_out.at[m, c],
            dst_ref=x_in.at[m, c],
            send_sem=send_sem.at[m, c],
            recv_sem=in_sem.at[m, c],
            device_id={"pp": me + 1},
            device_id_type=MESH,
        )

    def home_copy(m, c):
        return pltpu.make_async_remote_copy(
            src_ref=y_out.at[m, c],
            dst_ref=landed.at[c],
            send_sem=send_sem.at[m, c],
            recv_sem=res_sem.at[c],
            device_id={"pp": m},
            device_id_type=MESH,
        )

    weight_copies = [
        pltpu.make_async_copy(w_in_hbm, w_in, w_sem.at[0]),
        pltpu.make_async_copy(gr_hbm, gates.at[:, :, pl.ds(0, LANES)], w_sem.at[1]),
        pltpu.make_async_copy(gi_hbm, gates.at[:, :, pl.ds(LANES, LANES)], w_sem.at[2]),
        pltpu.make_async_copy(w_out_hbm, w_out, w_sem.at[3]),
    ]

    barrier = pltpu.get_barrier_semaphore()
    for step in range(1, stages):
        pl.semaphore_signal(
            barrier, inc=1, device_id={"pp": lax.rem(me + step, stages)}, device_id_type=MESH
        )

    @pl.when(me == 0)
    def _():
        for c in range(chunks):
            pltpu.make_async_copy(tokens.at[chunk_rows(c)], x_in.at[0, c], in_sem.at[0, c]).start()

    for copy in weight_copies:
        copy.start()
    rates[...] = -8.0 * (
        jnp.maximum(-decay_setting[...], 0.0)
        + jnp.log1p(jnp.exp(-jnp.abs(decay_setting[...])))
    )
    spikes[...] = jnp.broadcast_to(spike[...], (LANES, length)).T
    tails[...] = jnp.zeros_like(tails)
    carries[...] = jnp.zeros_like(carries)
    pl.semaphore_wait(barrier, stages - 1)

    @pl.when(me == 1)
    def _():
        for c in range(chunks):
            token_copy(c).start()

    for copy in weight_copies:
        copy.wait()

    def layer(m, c):
        hidden = x_in[m, c].astype(jnp.float32)
        squares = jnp.mean(hidden * hidden, axis=-1, keepdims=True)
        normed = (hidden * lax.rsqrt(squares + 1e-6) * scale[...]).astype(jnp.bfloat16)
        row_in_group = lax.broadcasted_iota(jnp.int32, (rows // GROUP, GROUP, LANES), 1)
        spiked = spikes[chunk_rows(c), :]
        pair = 2 * LANES
        for two in range(channels // pair):
            wide = slice(two * pair, (two + 1) * pair)
            mixed = jnp.dot(normed, w_in[:, wide], preferred_element_type=jnp.float32)
            mixed = mixed.astype(jnp.bfloat16).astype(jnp.float32)
            padded = jnp.concatenate([tails[m, :, wide], mixed], axis=0)
            tails[m, :, wide] = mixed[rows - GROUP :]
            conv = tap_bias[:, wide]
            for k in range(ntaps):
                start = GROUP - (ntaps - 1) + k
                conv = conv + padded[start : start + rows] * taps[k : k + 1, wide]
            conv = conv.astype(jnp.bfloat16)
            for half in range(2):
                g = 2 * two + half
                lanes = slice(g * LANES, (g + 1) * LANES)
                mine = conv[:, half * LANES : (half + 1) * LANES]
                z = jnp.dot(mine, gates[g], preferred_element_type=jnp.float32)
                recall = jax.nn.sigmoid(z[:, :LANES] + bias_r[:, lanes])
                inject = jax.nn.sigmoid(z[:, LANES:] + bias_i[:, lanes])
                log_decay = recall * rates[:, lanes] + spiked
                a = jnp.exp(log_decay)
                u = jnp.sqrt(one_minus_exp(2.0 * log_decay)) * inject * mine.astype(jnp.float32)
                a = a.reshape(rows // GROUP, GROUP, LANES)
                u = u.reshape(rows // GROUP, GROUP, LANES)
                for by in (1, 2, 4):
                    inside = row_in_group >= by
                    u = u + a * jnp.where(inside, pltpu.roll(u, by, 1), 0.0)
                    a = a * jnp.where(inside, pltpu.roll(a, by, 1), 1.0)
                carry = carries[m, :, lanes]
                parts = []
                for i in range(rows // GROUP):
                    h = a[i] * carry + u[i]
                    parts.append(h)
                    carry = jnp.broadcast_to(h[GROUP - 1 :], (GROUP, LANES))
                carries[m, :, lanes] = carry
                states[:, lanes] = jnp.concatenate(parts, axis=0).astype(jnp.bfloat16)
        projected = jnp.dot(states[...], w_out[...], preferred_element_type=jnp.float32)
        y_out[m, c] = (x_in[m, c].astype(jnp.float32) + projected).astype(jnp.bfloat16)

    def advance(i, _):
        m = i // chunks
        c = i % chunks

        @pl.when((me > 1) & (i == jnp.maximum(me - 2, 0)))
        def _():
            pl.semaphore_wait(go_sem, 1)
            for q in range(chunks):
                token_copy(q).start()

        @pl.when((me > 0) & (me < last) & (i == me + 0))
        def _():
            token_copy(GO_CHUNK).wait_send()
            pl.semaphore_signal(go_sem, inc=1, device_id={"pp": me + 1}, device_id_type=MESH)

        pltpu.make_async_copy(x_in.at[m, c], x_in.at[m, c], in_sem.at[m, c]).wait()
        layer(m, c)

        @pl.when(me < last)
        def _():
            forward_copy(m, c).start()

        @pl.when((me == last) & (m < last) & (m > 0))
        def _():
            home_copy(m, c).start()

        @pl.when((me == last) & (i >= DEFER) & (i < DEFER + chunks))
        def _():
            home_copy(0, i - DEFER).start()

        return 0

    lax.fori_loop(0, stages * chunks, advance, 0)

    def final_copy(source, c):
        return pltpu.make_async_copy(source, out.at[chunk_rows(c)], out_sem.at[c])

    @pl.when(me == last)
    def _():
        for c in range(chunks):
            final_copy(y_out.at[last, c], c).start()

    @pl.when(me < last)
    def _():
        for c in range(chunks):
            pltpu.make_async_copy(landed.at[c], landed.at[c], res_sem.at[c]).wait()
            final_copy(landed.at[c], c).start()

    @pl.when(me > 0)
    def _():
        for c in range(chunks):
            if c != GO_CHUNK:
                token_copy(c).wait_send()

    @pl.when(me == last)
    def _():
        token_copy(GO_CHUNK).wait_send()

    def drain(i, _):
        m = i // chunks
        c = i % chunks

        @pl.when(me < last)
        def _():
            forward_copy(m, c).wait_send()

        @pl.when((me == last) & (m < last))
        def _():
            home_copy(m, c).wait_send()

        return 0

    lax.fori_loop(0, stages * chunks, drain, 0)
    for c in range(chunks):
        final_copy(landed.at[c], c).wait()


def solution(mesh):
    stages = mesh.shape["pp"]

    def local(
        tokens, norm, w_in, taps, tap_bias, gr, br, gi, bi, decay_setting, spike, w_out
    ):
        length, width = tokens.shape[2:]
        channels = w_in.shape[2]
        blocks, wide = gr.shape[1:3]
        rows = length // CHUNKS
        vmem = pl.BlockSpec(memory_space=pltpu.VMEM)
        anywhere = pl.BlockSpec(memory_space=pl.ANY)
        result = pl.pallas_call(
            functools.partial(kernel, stages, CHUNKS),
            out_shape=jax.ShapeDtypeStruct((length, width), jnp.bfloat16),
            in_specs=[
                anywhere, vmem, anywhere, vmem, vmem, anywhere, vmem, anywhere, vmem, vmem, vmem,
                anywhere,
            ],
            out_specs=anywhere,
            scratch_shapes=[
                pltpu.VMEM((stages, CHUNKS, rows, width), jnp.bfloat16),
                pltpu.VMEM((stages, CHUNKS, rows, width), jnp.bfloat16),
                pltpu.VMEM((CHUNKS, rows, width), jnp.bfloat16),
                pltpu.VMEM((width, channels), jnp.bfloat16),
                pltpu.VMEM((channels, width), jnp.bfloat16),
                pltpu.VMEM((blocks, wide, 2 * wide), jnp.bfloat16),
                pltpu.VMEM((stages, GROUP, channels), jnp.float32),
                pltpu.VMEM((stages, GROUP, channels), jnp.float32),
                pltpu.VMEM((1, channels), jnp.float32),
                pltpu.VMEM((length, LANES), jnp.float32),
                pltpu.VMEM((rows, channels), jnp.bfloat16),
                pltpu.SemaphoreType.DMA((stages, CHUNKS)),
                pltpu.SemaphoreType.DMA((stages, CHUNKS)),
                pltpu.SemaphoreType.DMA((CHUNKS,)),
                pltpu.SemaphoreType.DMA((CHUNKS,)),
                pltpu.SemaphoreType.DMA((4,)),
                pltpu.SemaphoreType.DMA((CHUNKS,)),
                pltpu.SemaphoreType.REGULAR,
            ],
            compiler_params=pltpu.CompilerParams(
                collective_id=0, has_side_effects=True, vmem_limit_bytes=60 * 1024 * 1024
            ),
        )(
            tokens[0, 0], norm, w_in[0], taps[0], tap_bias, gr[0], br, gi[0], bi, decay_setting,
            spike, w_out[0],
        )
        return result[None, None]

    placed = (
        P("pp", ("fs", "tp"), None, None),
        P("pp", None),
        P("pp", None, None),
        P("pp", None, None),
        P("pp", None),
        P("pp", None, None, None),
        P("pp", None),
        P("pp", None, None, None),
        P("pp", None),
        P("pp", None),
        P("pp", None),
        P("pp", None, None),
    )
    return jax.shard_map(
        local,
        mesh=mesh,
        in_specs=placed,
        out_specs=P("pp", ("fs", "tp"), None, None),
        check_vma=False,
    )
```
